32 devices in a mesh: fs: 8 (over z, y), tp: 4 (over x, core).
Axes of the slice: x: 2, y: 2, z: 4, core: 2. Of those that a mesh axis runs over, the one named last changes fastest.
Arguments:
- tokens: bfloat16 [8192, 2048], P('fs', 'tp'), may hold values from -6 to 6
- mixer_gain: float32 [2048], replicated, may hold values from 0.1 to 1.9
- ffn_gain: float32 [2048], replicated, may hold values from 0.1 to 1.9
- w_outer: float32 [2048, 1024], P('fs', 'tp'), may hold values from -0.125 to 0.125
- w_inner: float32 [2048, 1024], P('fs', 'tp'), may hold values from -0.125 to 0.125
- w_value: float32 [2048, 1024], P('fs', 'tp'), may hold values from -0.125 to 0.125
- scale_outer: float32 [1, 1024], P(None, 'tp'), may hold values from 0.5 to 2
- scale_inner: float32 [1, 1024], P(None, 'tp'), may hold values from 0.5 to 2
- scale_value: float32 [1, 1024], P(None, 'tp'), may hold values from 0.5 to 2
- conv_taps: float32 [3, 1024], P(None, 'tp'), may hold values from -3.5 to 3.5
- w_mixout: float32 [1024, 2048], P('tp', 'fs'), may hold values from -0.1875 to 0.1875
- scale_mixout: float32 [1, 2048], P(None, 'fs'), may hold values from 0.5 to 2
- w_gate: float32 [2048, 5632], P('fs', 'tp'), may hold values from -0.125 to 0.125
- w_upward: float32 [2048, 5632], P('fs', 'tp'), may hold values from -0.125 to 0.125
- scale_gate: float32 [1, 5632], P(None, 'tp'), may hold values from 0.5 to 2
- scale_upward: float32 [1, 5632], P(None, 'tp'), may hold values from 0.5 to 2
- w_down: float32 [5632, 2048], P('tp', 'fs'), may hold values from -0.078125 to 0.078125
- scale_down: float32 [1, 2048], P(None, 'fs'), may hold values from 0.5 to 2
Outputs:
- block_out: bfloat16 [8192, 2048], P('fs', 'tp')
The draws below stay inside these ranges and needn't reach their ends.
All inputs are finite; a program needn't handle non-finite values.
Results may differ from the reference program's by a relative error of at most 0.019.
Values may be sent and summed in bfloat16 or wider, within the bound.
A program may use at most 128 MiB of HBM per device.

```python
import math
import jax
import jax.numpy as jnp
from jax import lax

MODEL = 2048
CHANNELS = 1024
HIDDEN_SIZE = 5632
TAPS = 3
SEQ_LEN = 128
TOKENS = 8192
N_TP = 4


def levels(rng, extent, pieces, low, high):
    def one(position, blocks):
        draws = jax.random.uniform(jax.random.fold_in(jax.random.fold_in(rng, 6), position), (blocks,), jnp.float32, low / len(pieces), high / len(pieces))
        return jnp.repeat(jnp.exp(draws), extent[position] // blocks).reshape((-1,) + (1,) * (len(extent) - position - 1))

    factor_of = one(*pieces[0])
    for cut in pieces[1:]:
        factor_of = factor_of * one(*cut)
    return factor_of


def scatter_about(rng, dims, deviation, reach, pieces=(), kind=jnp.bfloat16):
    result = jax.random.normal(rng, dims, jnp.float32) * deviation
    if len(pieces) > 0:
        result = levels(rng, dims, pieces, -0.22, 0.18) * result
    return jnp.clip(result, min=-reach, max=reach).astype(kind)


def setup_inputs(seed: int = 0) -> dict:
    splits = jax.random.split(jax.random.key(seed), 19)
    return {
        "tokens": scatter_about(splits[0], (TOKENS, MODEL), 1.0, 6.0, ((0, 8), (1, 4))),
        "mixer_gain": jnp.clip(1.0 + 0.18 * jax.random.normal(splits[1], (MODEL,), jnp.float32), 0.1, 1.9),
        "ffn_gain": jnp.clip(1.0 + 0.18 * jax.random.normal(splits[2], (MODEL,), jnp.float32), 0.1, 1.9),
        "w_outer": scatter_about(splits[3], (MODEL, CHANNELS), MODEL ** -0.5, 0.125, ((0, 8), (1, 4)), jnp.float32),
        "w_inner": scatter_about(splits[4], (MODEL, CHANNELS), MODEL ** -0.5, 0.125, ((0, 8), (1, 4)), jnp.float32),
        "w_value": scatter_about(splits[5], (MODEL, CHANNELS), MODEL ** -0.5, 0.125, ((0, 8), (1, 4)), jnp.float32),
        "scale_outer": jnp.clip(jnp.exp(math.log(2.0) - 1.3862944 * jax.random.uniform(splits[6], (1, CHANNELS), jnp.float32) ** levels(splits[6], (1, CHANNELS), ((1, 4),), -0.2, 0.2)), 0.5, 2.0),
        "scale_inner": jnp.clip(jnp.exp(math.log(2.0) - 1.3862944 * jax.random.uniform(splits[7], (1, CHANNELS), jnp.float32) ** levels(splits[7], (1, CHANNELS), ((1, 4),), -0.2, 0.2)), 0.5, 2.0),
        "scale_value": jnp.clip(jnp.exp(math.log(2.0) - 1.3862944 * jax.random.uniform(splits[8], (1, CHANNELS), jnp.float32) ** levels(splits[8], (1, CHANNELS), ((1, 4),), -0.2, 0.2)), 0.5, 2.0),
        "conv_taps": scatter_about(splits[9], (TAPS, CHANNELS), TAPS ** -0.5, 3.5, ((1, 4),), jnp.float32),
        "w_mixout": scatter_about(splits[10], (CHANNELS, MODEL), CHANNELS ** -0.5, 0.1875, ((0, 4), (1, 8)), jnp.float32),
        "scale_mixout": jnp.clip(jnp.exp(math.log(2.0) - 1.3862944 * jax.random.uniform(splits[11], (1, MODEL), jnp.float32) ** levels(splits[11], (1, MODEL), ((1, 8),), -0.2, 0.2)), 0.5, 2.0),
        "w_gate": scatter_about(splits[12], (MODEL, HIDDEN_SIZE), MODEL ** -0.5, 0.125, ((0, 8), (1, 4)), jnp.float32),
        "w_upward": scatter_about(splits[13], (MODEL, HIDDEN_SIZE), MODEL ** -0.5, 0.125, ((0, 8), (1, 4)), jnp.float32),
        "scale_gate": jnp.clip(jnp.exp(math.log(2.0) - 1.3862944 * jax.random.uniform(splits[14], (1, HIDDEN_SIZE), jnp.float32) ** levels(splits[14], (1, HIDDEN_SIZE), ((1, 4),), -0.2, 0.2)), 0.5, 2.0),
        "scale_upward": jnp.clip(jnp.exp(math.log(2.0) - 1.3862944 * jax.random.uniform(splits[15], (1, HIDDEN_SIZE), jnp.float32) ** levels(splits[15], (1, HIDDEN_SIZE), ((1, 4),), -0.2, 0.2)), 0.5, 2.0),
        "w_down": scatter_about(splits[16], (HIDDEN_SIZE, MODEL), HIDDEN_SIZE ** -0.5, 0.078125, ((0, 4), (1, 8)), jnp.float32),
        "scale_down": jnp.clip(jnp.exp(math.log(2.0) - 1.3862944 * jax.random.uniform(splits[17], (1, MODEL), jnp.float32) ** levels(splits[17], (1, MODEL), ((1, 8),), -0.2, 0.2)), 0.5, 2.0),
    }


def rms_scaled(full_rows, gain_vec):
    values = full_rows.astype(jnp.float32)
    inverse = lax.rsqrt(lax.optimization_barrier(jnp.mean(values * values, axis=-1, keepdims=True)) + 1e-06)
    return (values * inverse * gain_vec).astype(jnp.bfloat16)

def causal_taps(product, conv_taps):
    padded = jnp.pad(product, ((0, 0), (TAPS - 1, 0), (0, 0)))
    length = product.shape[1]
    summed = jnp.zeros(product.shape, jnp.float32)
    for tap_index in range(TAPS):
        summed = summed + conv_taps[tap_index] * padded[:, tap_index:tap_index + length, :]
    return summed

def reference(tokens, mixer_gain, ffn_gain, w_outer, w_inner, w_value, scale_outer, scale_inner, scale_value, conv_taps, w_mixout, scale_mixout, w_gate, w_upward, scale_gate, scale_upward, w_down, scale_down):
    normed = rms_scaled(tokens, mixer_gain)

    def project(weight, column_scale):
        return jnp.dot(normed, weight.astype(jnp.bfloat16), preferred_element_type=jnp.float32) * column_scale
    outer = project(w_outer, scale_outer)
    inner = project(w_inner, scale_inner)
    value = project(w_value, scale_value)
    product = (inner * value).reshape(-1, SEQ_LEN, CHANNELS)
    conv = causal_taps(product, conv_taps).reshape(-1, CHANNELS)
    mixed_out = (outer * conv).astype(jnp.bfloat16)
    mix_term = jnp.dot(mixed_out, w_mixout.astype(jnp.bfloat16), preferred_element_type=jnp.float32) * scale_mixout
    residual = (tokens.astype(jnp.float32) + mix_term).astype(jnp.bfloat16)
    normed_ffn = rms_scaled(residual, ffn_gain)
    gate_proj = jnp.dot(normed_ffn, w_gate.astype(jnp.bfloat16), preferred_element_type=jnp.float32) * scale_gate
    up_proj = jnp.dot(normed_ffn, w_upward.astype(jnp.bfloat16), preferred_element_type=jnp.float32) * scale_upward
    hidden = (jax.nn.silu(gate_proj) * up_proj).astype(jnp.bfloat16)
    down_bf = w_down.astype(jnp.bfloat16)
    block_width = HIDDEN_SIZE // N_TP

    def add_block(summed, block_index):
        offset = (block_index * block_width).astype(jnp.int32)
        left = lax.dynamic_slice_in_dim(hidden, offset, block_width, 1)
        right = lax.dynamic_slice_in_dim(down_bf, offset, block_width, 0)
        part = (jnp.dot(left, right, preferred_element_type=jnp.float32) * scale_down).astype(jnp.bfloat16)
        part = lax.optimization_barrier(part)
        return (summed + part.astype(jnp.float32), None)
    ffn_sum, _ = lax.scan(add_block, jnp.zeros(residual.shape, jnp.float32), jnp.arange(N_TP, dtype=jnp.int32))
    return (residual.astype(jnp.float32) + ffn_sum).astype(jnp.bfloat16)
```

```python
import jax
import jax.numpy as jnp
from jax import lax
from jax.sharding import PartitionSpec as P

SEQ_LEN = 128


def grid_of(count):
    inner = 1
    while (inner * 2) ** 2 <= count:
        inner *= 2
    return count // inner, inner


def gather_pieces(shard):
    count = lax.axis_size("fs")
    depth, width = grid_of(count)
    me = lax.axis_index("fs")
    zed, why = lax.div(me, width), lax.rem(me, width)

    def move(array, dz, dy):
        pairs = [
            (z * width + y, ((z + dz) % depth) * width + (y + dy) % width)
            for z in range(depth)
            for y in range(width)
        ]
        return lax.ppermute(array, "fs", pairs)

    def owner(dz, dy):
        return lax.rem(zed + dz_back(dz), depth) * width + lax.rem(why + width - dy, width)

    def dz_back(dz):
        return (-dz) % depth

    pieces = [(me, 0, shard)]
    if depth == 4 and width == 2:
        half = shard.shape[0] // 2
        beside = move(shard, 0, 1)
        below, above = move(shard, 1, 0), move(shard, -1, 0)
        far_low, far_high = move(below[:half], 1, 0), move(above[half:], -1, 0)
        pieces += [(owner(0, 1), 0, beside), (owner(1, 0), 0, below), (owner(-1, 0), 0, above)]
        pieces += [
            (owner(1, 1), 0, move(beside, 1, 0)),
            (owner(-1, 1), 0, move(beside, -1, 0)),
            (owner(2, 0), 0, far_low),
            (owner(2, 0), half, far_high),
            (owner(2, 1), 0, move(far_low, 0, 1)),
            (owner(2, 1), half, move(far_high, 0, 1)),
        ]
        return pieces
    column = [(0, shard)]
    for step in range(1, width):
        column.append((step, move(column[-1][1], 0, 1)))
    for dy, array in column:
        low = high = array
        if dy:
            pieces.append((owner(0, dy), 0, array))
        for step in range(1, depth):
            if step % 2:
                low = move(low, 1, 0)
                pieces.append((owner((step + 1) // 2, dy), 0, low))
            else:
                high = move(high, -1, 0)
                pieces.append((owner(-(step // 2), dy), 0, high))
    return pieces


def assemble(pieces, shard):
    full = jnp.zeros((lax.axis_size("fs"),) + shard.shape, shard.dtype)
    for who, first_row, piece in pieces:
        full = lax.dynamic_update_slice(full, piece[None], (who, first_row, 0))
    return full


def gather_fs(shard):
    pieces = gather_pieces(shard)
    return assemble(pieces, shard), sum(piece[0, 0] for _, _, piece in pieces[1:4])


def after(weights, token):
    return (weights + 0.0 * token.astype(jnp.float32)).astype(jnp.bfloat16)


def gather_small(shard):
    count = lax.axis_size("fs")
    me = lax.axis_index("fs")
    full = jnp.zeros((count,) + shard.shape, shard.dtype)
    full = lax.dynamic_update_slice(full, shard[None], (me, 0, 0))
    for step in range(1, count):
        piece = lax.ppermute(shard, "fs", [(i, (i + step) % count) for i in range(count)])
        full = lax.dynamic_update_slice(full, piece[None], (lax.rem(me + count - step, count), 0, 0))
    return full


def rms_scaled(full_rows, gain_vec):
    values = full_rows.astype(jnp.float32)
    inverse = lax.rsqrt(jnp.mean(values * values, axis=-1, keepdims=True) + 1e-06)
    return (values * inverse * gain_vec).astype(jnp.bfloat16)


def add_rows(left, w_piece):
    return jnp.dot(left, w_piece, preferred_element_type=jnp.float32)


def causal_taps(product, conv_taps):
    padded = jnp.pad(product, ((0, 0), (conv_taps.shape[0] - 1, 0), (0, 0)))
    length = product.shape[1]
    summed = jnp.zeros(product.shape, jnp.float32)
    for tap_index in range(conv_taps.shape[0]):
        summed = summed + conv_taps[tap_index] * padded[:, tap_index : tap_index + length, :]
    return summed


def per_device(
    tokens,
    mixer_gain,
    ffn_gain,
    w_outer,
    w_inner,
    w_value,
    scale_outer,
    scale_inner,
    scale_value,
    conv_taps,
    w_mixout,
    scale_mixout,
    w_gate,
    w_upward,
    scale_gate,
    scale_upward,
    w_down,
    scale_down,
):
    bf16 = jnp.bfloat16
    full_rows = lax.all_gather(tokens, "tp", axis=1, tiled=True)
    tok_count = tokens.shape[0]
    feature_count = tokens.shape[1]
    local_channels = w_outer.shape[1]
    local_hidden = w_gate.shape[1]
    mixer_shard = jnp.concatenate([w_outer, w_inner, w_value], axis=1).astype(bf16)
    mixer_full, mixer_token = gather_fs(mixer_shard)
    mixer_full = mixer_full.reshape(-1, 3 * local_channels)
    mixout_cols, _ = gather_fs(w_mixout.astype(bf16))
    gate_full, gate_token = gather_fs(after(w_gate, mixer_token))
    up_full, up_token = gather_fs(after(w_upward, gate_token))
    down_cols, _ = gather_fs(after(w_down, up_token))
    gate_full = gate_full.reshape(-1, local_hidden)
    up_full = up_full.reshape(-1, local_hidden)
    scales = gather_small(jnp.concatenate([scale_mixout, scale_down], axis=0))
    blocks = scales.shape[0]
    block = scales.shape[2]

    normed = rms_scaled(full_rows, mixer_gain)
    projected = add_rows(normed, mixer_full)
    outer = projected[:, :local_channels] * scale_outer
    inner = projected[:, local_channels : 2 * local_channels] * scale_inner
    value = projected[:, 2 * local_channels :] * scale_value
    product = (inner * value).reshape(tok_count // SEQ_LEN, SEQ_LEN, local_channels)
    conv = causal_taps(product, conv_taps).reshape(tok_count, local_channels)
    mixed_out = (outer * conv).astype(bf16)
    mixed_all = lax.all_gather(mixed_out, "tp", axis=1, tiled=True)
    mixout_all = lax.all_gather(mixout_cols, "tp", axis=1, tiled=True)
    residual_rows = jnp.concatenate(
        [
            (
                full_rows[:, b * block : (b + 1) * block].astype(jnp.float32)
                + add_rows(mixed_all, mixout_all[b]) * scales[b, 0]
            ).astype(bf16)
            for b in range(blocks)
        ],
        axis=1,
    )
    residual = lax.dynamic_slice_in_dim(
        residual_rows, lax.axis_index("tp") * feature_count, feature_count, 1
    )
    normed_ffn = rms_scaled(residual_rows, ffn_gain)
    gate_proj = add_rows(normed_ffn, gate_full)
    up_proj = add_rows(normed_ffn, up_full)
    hidden = (jax.nn.silu(gate_proj * scale_gate) * (up_proj * scale_upward)).astype(bf16)
    down_terms = jnp.concatenate(
        [(add_rows(hidden, down_cols[b]) * scales[b, 1]).astype(bf16) for b in range(blocks)],
        axis=1,
    )
    ffn_share = lax.psum_scatter(down_terms, "tp", scatter_dimension=1, tiled=True)
    return (residual.astype(jnp.float32) + ffn_share.astype(jnp.float32)).astype(bf16)


def solution(mesh):
    in_specs = (
        P("fs", "tp"),
        P(),
        P(),
        P("fs", "tp"),
        P("fs", "tp"),
        P("fs", "tp"),
        P(None, "tp"),
        P(None, "tp"),
        P(None, "tp"),
        P(None, "tp"),
        P("tp", "fs"),
        P(None, "fs"),
        P("fs", "tp"),
        P("fs", "tp"),
        P(None, "tp"),
        P(None, "tp"),
        P("tp", "fs"),
        P(None, "fs"),
    )
    out_specs = P("fs", "tp")
    return jax.shard_map(
        per_device, mesh=mesh, in_specs=in_specs, out_specs=out_specs, check_vma=False
    )
```

```python
import jax
import jax.numpy as jnp
from jax import lax
from jax.experimental import pallas as pl
from jax.experimental.pallas import tpu as pltpu
from jax.sharding import PartitionSpec as P

SEQ_LEN = 128


def rms_scaled(full_rows, gain_vec):
    values = full_rows.astype(jnp.float32)
    inverse = lax.rsqrt(jnp.mean(values * values, axis=-1, keepdims=True) + 1e-06)
    return (values * inverse * gain_vec).astype(jnp.bfloat16)


def add_rows(left, w_piece):
    return jnp.dot(left, w_piece, preferred_element_type=jnp.float32)


def causal_taps(product, conv_taps):
    padded = jnp.pad(product, ((0, 0), (conv_taps.shape[0] - 1, 0), (0, 0)))
    length = product.shape[1]
    summed = jnp.zeros(product.shape, jnp.float32)
    for tap_index in range(conv_taps.shape[0]):
        summed = summed + conv_taps[tap_index] * padded[:, tap_index : tap_index + length, :]
    return summed


DEPTH, WIDTH, TP = 4, 2, 4
ROWS = 256
MESH = pl.DeviceIdType.MESH


def block_kernel(
    tokens, mixer_gain, ffn_gain, s_mixer, taps, s_gate, s_up,
    h_scales, h_mixer, h_mixout, h_gate, h_up, h_down,
    out, residual_own,
    rows, mixer, mixout, gate, up, down, scales, mixed, hidden,
    fs_send, fs_recv, tp_send, tp_recv, local_sem,
):
    f32, bf16 = jnp.float32, jnp.bfloat16
    me, tp = lax.axis_index("fs"), lax.axis_index("tp")
    zed, why = lax.div(me, WIDTH), lax.rem(me, WIDTH)
    near_x, core = lax.div(tp, 2), lax.rem(tp, 2)

    def at(dz, dy):
        return lax.rem(zed + dz + DEPTH, DEPTH) * WIDTH + lax.rem(why + dy, WIDTH)

    beside, above, below = at(0, 1), at(1, 0), at(-1, 0)
    sibling = near_x * 2 + (1 - core)
    across = (1 - near_x) * 2 + core

    barrier = pltpu.get_barrier_semaphore()
    for peer in (beside, above, below):
        pl.semaphore_signal(barrier, inc=1, device_id={"fs": peer}, device_id_type=MESH)
    for peer in (sibling, across):
        pl.semaphore_signal(barrier, inc=1, device_id={"tp": peer}, device_id_type=MESH)
    pl.semaphore_wait(barrier, 5)

    shards = (h_scales, h_mixer, h_mixout, h_gate, h_up, h_down)
    fulls = (scales, mixer, mixout, gate, up, down)
    by_columns = (False, False, True, False, False, True)

    def slot(w, owner, part):
        height, wide = shards[w].shape
        first, size = 0, height
        if part is not None:
            size = height // 2
            first = part * size
        if by_columns[w]:
            base = tp * height if w == 2 else 0
            start = base + first
            if w == 2:
                start = pl.multiple_of(start, 128)
            return fulls[w].at[pl.ds(start, size), pl.ds(pl.multiple_of(owner * wide, wide), wide)]
        return fulls[w].at[pl.ds(pl.multiple_of(owner * height + first, size), size), :]

    kinds = (
        ((0, 0), None, beside), ((0, 0), None, above), ((0, 0), None, below),
        ((0, 1), None, above), ((0, 1), None, below),
        ((-1, 0), 0, above), ((1, 0), 1, below),
        ((2, 0), 0, beside), ((2, 0), 1, beside),
    )

    def copy(w, k):
        (dz, dy), part, target = kinds[k]
        place = slot(w, at(dz, dy), part)
        return pltpu.make_async_remote_copy(
            src_ref=shards[w] if k < 3 else place,
            dst_ref=place,
            send_sem=fs_send.at[w, k],
            recv_sem=fs_recv.at[w, k],
            device_id={"fs": target},
            device_id_type=MESH,
        )

    def own(w):
        return pltpu.make_async_copy(shards[w], slot(w, me, None), local_sem.at[w])

    def first(w):
        for k in (0, 1, 2):
            copy(w, k).start()
        own(w).start()

    def second(w):
        copy(w, 1).wait_recv()
        copy(w, 5).start()
        copy(w, 2).wait_recv()
        copy(w, 6).start()
        copy(w, 0).wait_recv()
        copy(w, 3).start()
        copy(w, 4).start()

    def third(w):
        copy(w, 5).wait_recv()
        copy(w, 7).start()
        copy(w, 6).wait_recv()
        copy(w, 8).start()

    def finish(w):
        for k in (3, 4, 7, 8):
            copy(w, k).wait_recv()
        own(w).wait()

    def tp_slot(a, owner):
        if a == 0:
            wide = tokens.shape[1]
            return rows.at[:, pl.ds(pl.multiple_of(owner * wide, wide), wide)]
        if a == 1:
            wide = mixed.shape[1] // TP
            return mixed.at[:, pl.ds(pl.multiple_of(owner * wide, wide), wide)]
        height = mixout.shape[0] // TP
        return mixout.at[pl.ds(pl.multiple_of(owner * height, height), height), :]

    def tp_copy(a, k):
        owner, target = ((tp, sibling), (tp, across), (across, sibling))[k]
        place = tp_slot(a, owner)
        return pltpu.make_async_remote_copy(
            src_ref=tokens if a == 0 and k < 2 else place,
            dst_ref=place,
            send_sem=tp_send.at[a, k],
            recv_sem=tp_recv.at[a, k],
            device_id={"tp": target},
            device_id_type=MESH,
        )

    def tp_first(a):
        tp_copy(a, 1).start()
        tp_copy(a, 0).start()

    def tp_second(a):
        tp_copy(a, 1).wait_recv()
        tp_copy(a, 2).start()

    def tp_finish(a):
        tp_copy(a, 0).wait_recv()
        tp_copy(a, 2).wait_recv()

    own_tokens = pltpu.make_async_copy(tokens, tp_slot(0, tp), local_sem.at[6])
    tp_first(0)
    own_tokens.start()
    for w in (1, 2, 0, 3):
        first(w)
    second(1)
    second(2)
    second(0)
    first(4)
    third(1)
    third(2)
    third(0)
    second(3)
    first(5)
    tp_second(0)
    finish(2)
    tp_first(2)
    finish(1)
    tp_finish(0)
    own_tokens.wait()

    count = tokens.shape[0] // ROWS
    chan = mixed.shape[1] // TP

    def tile(i):
        return pl.ds(pl.multiple_of(i * ROWS, ROWS), ROWS)

    def normalised(values, gain):
        inverse = lax.rsqrt(jnp.mean(values * values, axis=-1, keepdims=True) + 1e-06)
        return (values * inverse * gain[...]).astype(bf16)

    @pl.loop(0, count)
    def _(i):
        normed = normalised(rows[tile(i), :].astype(f32), mixer_gain)
        three = jnp.dot(normed, mixer[...], preferred_element_type=f32) * s_mixer[...]
        product = three[:, chan : 2 * chan] * three[:, 2 * chan :]
        place = lax.rem(lax.broadcasted_iota(jnp.int32, product.shape, 0), SEQ_LEN)
        total = jnp.zeros_like(product)
        last = taps.shape[0] - 1
        for j in range(taps.shape[0]):
            back = last - j
            moved = product
            if back:
                moved = jnp.where(place >= back, pltpu.roll(product, back, 0), 0.0)
            total = total + taps[j : j + 1, :] * moved
        mixed[tile(i), pl.ds(pl.multiple_of(tp * chan, chan), chan)] = (
            three[:, :chan] * total
        ).astype(bf16)

    tp_first(1)
    third(3)
    second(4)
    tp_second(2)
    tp_second(1)
    finish(0)
    tp_finish(2)
    tp_finish(1)
    for k in range(3):
        tp_copy(0, k).wait_send()

    block = scales.shape[1]
    blocks = DEPTH * WIDTH

    def scale_row(which):
        return jnp.concatenate(
            [scales[b * 16 + which * 8 : b * 16 + which * 8 + 1, :] for b in range(blocks)], axis=1
        )

    feat = tokens.shape[1]

    @pl.loop(0, count)
    def _(i):
        term = jnp.dot(mixed[tile(i), :], mixout[...], preferred_element_type=f32) * scale_row(0)
        residual = (rows[tile(i), :].astype(f32) + term).astype(bf16)
        rows[tile(i), :] = residual
        residual_own[tile(i), :] = rows[tile(i), pl.ds(pl.multiple_of(tp * feat, feat), feat)]
        rows[tile(i), :] = normalised(residual.astype(f32), ffn_gain)

    third(4)
    second(5)
    finish(3)
    finish(4)

    @pl.loop(0, count)
    def _(i):
        gate_part = jnp.dot(rows[tile(i), :], gate[...], preferred_element_type=f32) * s_gate[...]
        up_part = jnp.dot(rows[tile(i), :], up[...], preferred_element_type=f32) * s_up[...]
        hidden[tile(i), :] = (gate_part / (1.0 + jnp.exp(-gate_part)) * up_part).astype(bf16)

    third(5)
    finish(5)

    @pl.loop(0, count)
    def _(i):
        term = jnp.dot(hidden[tile(i), :], down[...], preferred_element_type=f32) * scale_row(1)
        out[tile(i), :] = term.astype(bf16)

    for w in range(6):
        for k in range(9):
            copy(w, k).wait_send()
    for a in (1, 2):
        for k in range(3):
            tp_copy(a, k).wait_send()


def fused_device(
    tokens,
    mixer_gain,
    ffn_gain,
    w_outer,
    w_inner,
    w_value,
    scale_outer,
    scale_inner,
    scale_value,
    conv_taps,
    w_mixout,
    scale_mixout,
    w_gate,
    w_upward,
    scale_gate,
    scale_upward,
    w_down,
    scale_down,
):
    bf16 = jnp.bfloat16
    count, feat = tokens.shape
    model = mixer_gain.shape[0]
    chan = w_outer.shape[1]
    units = w_gate.shape[1]
    cols = w_down.shape[1]
    shard = jnp.concatenate([w_outer, w_inner, w_value], axis=1).astype(bf16)
    s_mixer = jnp.concatenate([scale_outer, scale_inner, scale_value], axis=1)
    scale_shard = jnp.concatenate(
        [jnp.broadcast_to(scale_mixout, (8, cols)), jnp.broadcast_to(scale_down, (8, cols))], axis=0
    )
    vmem = pl.BlockSpec(memory_space=pltpu.VMEM)
    dma = pltpu.SemaphoreType.DMA
    terms, residual = pl.pallas_call(
        block_kernel,
        out_shape=(
            jax.ShapeDtypeStruct((count, model), bf16),
            jax.ShapeDtypeStruct((count, feat), bf16),
        ),
        in_specs=[vmem] * 13,
        out_specs=(vmem, vmem),
        scratch_shapes=[
            pltpu.VMEM((count, model), bf16),
            pltpu.VMEM((model, 3 * chan), bf16),
            pltpu.VMEM((TP * chan, model), bf16),
            pltpu.VMEM((model, units), bf16),
            pltpu.VMEM((model, units), bf16),
            pltpu.VMEM((units, model), bf16),
            pltpu.VMEM((16 * DEPTH * WIDTH, cols), jnp.float32),
            pltpu.VMEM((count, TP * chan), bf16),
            pltpu.VMEM((count, units), bf16),
            dma((6, 9)),
            dma((6, 9)),
            dma((3, 3)),
            dma((3, 3)),
            dma((7,)),
        ],
        compiler_params=pltpu.CompilerParams(
            collective_id=0, has_side_effects=True, vmem_limit_bytes=62 * 1024 * 1024
        ),
    )(
        tokens, mixer_gain[None], ffn_gain[None], s_mixer, conv_taps, scale_gate, scale_upward,
        scale_shard, shard, w_mixout.astype(bf16), w_gate.astype(bf16), w_upward.astype(bf16),
        w_down.astype(bf16),
    )
    share = lax.psum_scatter(terms, "tp", scatter_dimension=1, tiled=True)
    return (residual.astype(jnp.float32) + share.astype(jnp.float32)).astype(bf16)


def plain_device(
    tokens,
    mixer_gain,
    ffn_gain,
    w_outer,
    w_inner,
    w_value,
    scale_outer,
    scale_inner,
    scale_value,
    conv_taps,
    w_mixout,
    scale_mixout,
    w_gate,
    w_upward,
    scale_gate,
    scale_upward,
    w_down,
    scale_down,
):
    full_rows = lax.all_gather(tokens, "tp", axis=1, tiled=True)
    normed = rms_scaled(full_rows, mixer_gain)
    tok_count = tokens.shape[0]
    local_channels = w_outer.shape[1]

    def add_one(w_piece):
        return add_rows(normed, w_piece)

    outer_bf = w_outer.astype(jnp.bfloat16)
    inner_bf = w_inner.astype(jnp.bfloat16)
    value_bf = w_value.astype(jnp.bfloat16)
    outer = add_one(lax.all_gather(outer_bf, "fs", axis=0, tiled=True))
    inner = add_one(lax.all_gather(inner_bf, "fs", axis=0, tiled=True))
    value = add_one(lax.all_gather(value_bf, "fs", axis=0, tiled=True))
    outer = outer * scale_outer
    product = inner * scale_inner * (value * scale_value)
    product = product.reshape(tok_count // SEQ_LEN, SEQ_LEN, local_channels)
    conv = causal_taps(product, conv_taps).reshape(tok_count, local_channels)
    mixed_out = (outer * conv).astype(jnp.bfloat16)
    mixout_scales, down_scales = (
        lax.all_gather(scale_mixout, "fs", axis=1, tiled=True),
        lax.all_gather(scale_down, "fs", axis=1, tiled=True),
    )
    mixout_bf = w_mixout.astype(jnp.bfloat16)
    mixed_all = lax.all_gather(mixed_out, "tp", axis=1, tiled=True)
    mixout_cols = lax.all_gather(mixout_bf, "fs", axis=1, tiled=True)
    mixout_all = lax.all_gather(mixout_cols, "tp", axis=0, tiled=True)
    mix_term = jnp.dot(mixed_all, mixout_all, preferred_element_type=jnp.float32) * mixout_scales
    residual_rows = (full_rows.astype(jnp.float32) + mix_term).astype(jnp.bfloat16)
    feature_count = tokens.shape[1]
    residual = lax.dynamic_slice_in_dim(
        residual_rows, lax.axis_index("tp") * feature_count, feature_count, 1
    )
    normed_ffn = rms_scaled(residual_rows, ffn_gain)
    gate_proj = add_rows(
        normed_ffn, lax.all_gather(w_gate.astype(jnp.bfloat16), "fs", axis=0, tiled=True)
    )
    up_proj = add_rows(
        normed_ffn, lax.all_gather(w_upward.astype(jnp.bfloat16), "fs", axis=0, tiled=True)
    )
    hidden = (jax.nn.silu(gate_proj * scale_gate) * (up_proj * scale_upward)).astype(jnp.bfloat16)
    down_terms = (
        jnp.dot(
            hidden,
            lax.all_gather(w_down.astype(jnp.bfloat16), "fs", axis=1, tiled=True),
            preferred_element_type=jnp.float32,
        )
        * down_scales
    )
    ffn_share = lax.psum_scatter(
        down_terms.astype(jnp.bfloat16), "tp", scatter_dimension=1, tiled=True
    ).astype(jnp.float32)
    return (residual.astype(jnp.float32) + ffn_share).astype(jnp.bfloat16)


def solution(mesh):
    in_specs = (
        P("fs", "tp"),
        P(),
        P(),
        P("fs", "tp"),
        P("fs", "tp"),
        P("fs", "tp"),
        P(None, "tp"),
        P(None, "tp"),
        P(None, "tp"),
        P(None, "tp"),
        P("tp", "fs"),
        P(None, "fs"),
        P("fs", "tp"),
        P("fs", "tp"),
        P(None, "tp"),
        P(None, "tp"),
        P("tp", "fs"),
        P(None, "fs"),
    )
    out_specs = P("fs", "tp")
    chosen = fused_device if (mesh.shape["fs"], mesh.shape["tp"]) == (8, 4) else plain_device
    return jax.shard_map(
        chosen, mesh=mesh, in_specs=in_specs, out_specs=out_specs, check_vma=False
    )
```
